32 devices in a mesh: rep: 2 (over x), fs: 4 (over z), tp: 4 (over y, core).
Axes of the slice: x: 2, y: 2, z: 4, core: 2. Of those that a mesh axis runs over, the one named last changes fastest.
Arguments:
- tokens: bfloat16 [1024, 4096], P(('rep', 'fs'), 'tp'), may hold values from -6 to 6
- mixer_gain: float32 [4096], replicated, may hold values from 0.75 to 1.25
- gate_proj: bfloat16 [4096, 2048], P('fs', 'tp'), may hold values from -0.09375 to 0.09375
- value_proj: bfloat16 [4096, 2048], P('fs', 'tp'), may hold values from -0.09375 to 0.09375
- value_gain: float32 [16, 128], P('tp'), may hold values from 0.75 to 1.25
- spatial_mix: bfloat16 [16, 128, 128], P('tp', 'fs'), may hold values from -0.5 to 0.5
- spatial_bias: float32 [16, 128], P('tp'), may hold values from 0.5 to 1.5
- head_gain: float32 [16, 128], P('tp'), may hold values from 0.75 to 1.25
- merge_proj: bfloat16 [2048, 4096], P('tp', 'fs'), may hold values from -0.125 to 0.125
- ffn_gain: float32 [4096], replicated, may hold values from 0.25 to 1.75
- gate_up: bfloat16 [4096, 11008], P('fs', 'tp'), may hold values from -0.09375 to 0.09375
- value_up: bfloat16 [4096, 11008], P('fs', 'tp'), may hold values from -0.09375 to 0.09375
- gate_kernel: float32 [3, 11008], P(None, 'tp'), may hold values from -3.5 to 3.5
- value_kernel: float32 [3, 11008], P(None, 'tp'), may hold values from -3.5 to 3.5
- gate_offset: float32 [11008], P('tp'), may hold values from -0.6 to 0.6
- value_offset: float32 [11008], P('tp'), may hold values from -1.8 to 1.8
- down_proj: bfloat16 [11008, 4096], P('tp', 'fs'), may hold values from -0.0546875 to 0.0546875
Outputs:
- layer_out: bfloat16 [1024, 4096], P(('rep', 'fs'), 'tp')
The draws below stay inside these ranges and needn't reach their ends.
All inputs are finite; a program needn't handle non-finite values.
Results may differ from the reference program's by a relative error of at most 0.02.
Values may be sent and summed in bfloat16 or wider, within the bound.
A program may use at most 128 MiB of HBM per device.

```python
import jax
import jax.numpy as jnp
from jax import lax

D = 4096
HEADS = 16
HEAD_DIM = 128
SEQ_LEN = 128
FF = 11008
DG = 2048
TOKENS = 1024


def shard_levels(own_key, extent, shards, smallest, top_value):
    level = 1.0
    for axis_at, blocks in shards:
        steps = jax.random.uniform(jax.random.fold_in(jax.random.fold_in(own_key, 6), axis_at), (blocks,), jnp.float32, smallest / len(shards), top_value / len(shards))
        level = level * jnp.repeat(jnp.exp(steps), extent[axis_at] // blocks).reshape((-1,) + (1,) * (len(extent) - 1 - axis_at))
    return level


def scatter_about(own_key, shape, deviation, bound, cuts=(), dtype=jnp.bfloat16):
    drawn = deviation * jax.random.normal(own_key, shape, jnp.float32)
    if cuts:
        drawn = drawn * shard_levels(own_key, shape, cuts, -0.22, 0.18)
    return jnp.clip(drawn, -bound, bound).astype(dtype)


def setup_inputs(seed: int = 0) -> dict:
    keys = jax.random.split(jax.random.key(seed), 18)
    tokens = scatter_about(keys[0], (TOKENS, D), 1.0, 6.0, ((0, 8), (1, 4)))
    mixer_gain = jnp.clip(1.0 + 0.05 * jax.random.normal(keys[1], (D,), jnp.float32), 0.75, 1.25)
    gate_proj = scatter_about(keys[2], (D, DG), D ** -0.5, 0.09375, ((0, 4), (1, 4)))
    value_proj = scatter_about(keys[3], (D, DG), D ** -0.5, 0.09375, ((0, 4), (1, 4)))
    value_gain = jnp.clip(1.0 + 0.05 * jax.random.normal(keys[4], (HEADS, HEAD_DIM), jnp.float32), 0.75, 1.25)
    spatial_mix = scatter_about(keys[5], (HEADS, SEQ_LEN, SEQ_LEN), SEQ_LEN ** -0.5, 0.5, ((0, 4), (1, 4)))
    spatial_bias = jnp.clip(1.0 + 0.1 * jax.random.normal(keys[6], (HEADS, SEQ_LEN), jnp.float32), 0.5, 1.5)
    head_gain = jnp.clip(1.0 + 0.05 * jax.random.normal(keys[7], (HEADS, HEAD_DIM), jnp.float32), 0.75, 1.25)
    merge_proj = scatter_about(keys[8], (DG, D), DG ** -0.5, 0.125, ((0, 4), (1, 4)))
    ffn_gain = jnp.clip(1.0 + 0.15 * jax.random.normal(keys[9], (D,), jnp.float32), 0.25, 1.75)
    gate_up = scatter_about(keys[10], (D, FF), D ** -0.5, 0.09375, ((0, 4), (1, 4)))
    value_up = scatter_about(keys[11], (D, FF), D ** -0.5, 0.09375, ((0, 4), (1, 4)))
    gate_kernel = scatter_about(keys[12], (3, FF), 3 ** -0.5, 3.5, ((1, 4),), jnp.float32)
    value_kernel = scatter_about(keys[13], (3, FF), 3 ** -0.5, 3.5, ((1, 4),), jnp.float32)
    gate_offset = scatter_about(keys[14], (FF,), 0.1, 0.6, ((0, 4),), jnp.float32)
    value_offset = scatter_about(keys[15], (FF,), 0.3, 1.8, ((0, 4),), jnp.float32)
    down_proj = scatter_about(keys[16], (FF, D), FF ** -0.5, 0.0546875, ((0, 4), (1, 4)))
    return {"tokens": tokens, "mixer_gain": mixer_gain, "gate_proj": gate_proj, "value_proj": value_proj, "value_gain": value_gain, "spatial_mix": spatial_mix, "spatial_bias": spatial_bias, "head_gain": head_gain, "merge_proj": merge_proj, "ffn_gain": ffn_gain, "gate_up": gate_up, "value_up": value_up, "gate_kernel": gate_kernel, "value_kernel": value_kernel, "gate_offset": gate_offset, "value_offset": value_offset, "down_proj": down_proj}


epsilon = 1e-06

def normalize(values, gain):
    values = values.astype(jnp.float32)
    scaled = values * lax.rsqrt(lax.optimization_barrier(jnp.mean(values * values, axis=-1, keepdims=True)) + epsilon)
    return scaled * gain

def rounded(values):
    return lax.optimization_barrier(values.astype(jnp.bfloat16)).astype(jnp.float32)

def gelu_exact(values):
    return jax.nn.gelu(values, approximate=False)

def convolve(values, kernel, offset, length):
    total_rows, width = values.shape
    blocks = values.reshape(total_rows // length, length, width)
    padded = jnp.pad(blocks, ((0, 0), (1, 1), (0, 0)))
    result = offset + padded[:, 0:length] * kernel[0] + padded[:, 1:length + 1] * kernel[1] + padded[:, 2:] * kernel[2]
    return result.reshape(total_rows, width)

def reference(tokens, mixer_gain, gate_proj, value_proj, value_gain, spatial_mix, spatial_bias, head_gain, merge_proj, ffn_gain, gate_up, value_up, gate_kernel, value_kernel, gate_offset, value_offset, down_proj):
    total_rows = tokens.shape[0]
    seqs = total_rows // SEQ_LEN
    normed = normalize(tokens, mixer_gain).astype(jnp.bfloat16)
    gated = gelu_exact(rounded(jnp.dot(normed, gate_proj, preferred_element_type=jnp.float32)))
    spread = gelu_exact(rounded(jnp.dot(normed, value_proj, preferred_element_type=jnp.float32)))
    spread = normalize(spread.reshape(seqs, SEQ_LEN, HEADS, HEAD_DIM), value_gain).astype(jnp.bfloat16)
    mixed = jnp.einsum('hij,njhd->nihd', spatial_mix.astype(jnp.float32), spread.astype(jnp.float32), precision=lax.Precision.HIGHEST)
    mixed = mixed + spatial_bias.T[None, :, :, None]
    joined = gated.reshape(seqs, SEQ_LEN, HEADS, HEAD_DIM) * mixed
    merged = normalize(joined, head_gain).astype(jnp.bfloat16).reshape(total_rows, DG)
    branch = jnp.dot(merged, merge_proj, preferred_element_type=jnp.float32)
    hidden = (tokens.astype(jnp.float32) + branch).astype(jnp.bfloat16)
    normed_ffn = normalize(hidden, ffn_gain).astype(jnp.bfloat16)
    upper_gate = rounded(jnp.dot(normed_ffn, gate_up, preferred_element_type=jnp.float32))
    upper_value = rounded(jnp.dot(normed_ffn, value_up, preferred_element_type=jnp.float32))
    conv_gate = convolve(upper_gate, gate_kernel, gate_offset, SEQ_LEN)
    conv_value = convolve(upper_value, value_kernel, value_offset, SEQ_LEN)
    active = (gelu_exact(conv_gate) * conv_value).astype(jnp.bfloat16)
    change = jnp.dot(active, down_proj, preferred_element_type=jnp.float32)
    return (hidden.astype(jnp.float32) + change).astype(jnp.bfloat16)
```

```python
import jax
import jax.numpy as jnp
from jax import lax
from jax.sharding import PartitionSpec as P

epsilon = 1e-06


def normalize(values, gain):
    values = values.astype(jnp.float32)
    scaled = values * lax.rsqrt(jnp.mean(values * values, axis=-1, keepdims=True) + epsilon)
    return scaled * gain


def gelu_exact(values):
    return jax.nn.gelu(values, approximate=False)


def convolve(values, kernel, offset, length):
    total_rows, width = values.shape
    blocks = values.reshape(total_rows // length, length, width)
    padded = jnp.pad(blocks, ((0, 0), (1, 1), (0, 0)))
    result = (
        offset
        + padded[:, 0:length] * kernel[0]
        + padded[:, 1 : length + 1] * kernel[1]
        + padded[:, 2:] * kernel[2]
    )
    return result.reshape(total_rows, width)


def dot(a, b):
    return jnp.dot(a, b, preferred_element_type=jnp.float32).astype(jnp.bfloat16)


def swap(block, fs, tp):
    if fs == tp:
        pairs = [(a * tp + b, b * tp + a) for a in range(fs) for b in range(tp)]
        return lax.ppermute(block, ("fs", "tp"), pairs)
    wide = lax.all_gather(block, "tp", axis=1, tiled=True)
    tall = lax.all_to_all(wide, "fs", 1, 0, tiled=True)
    rows = tall.shape[0] // tp
    return lax.dynamic_slice_in_dim(tall, lax.axis_index("tp") * rows, rows, 0)


def swap_back(block, fs, tp):
    if fs == tp:
        return swap(block, fs, tp)
    tall = lax.all_gather(block, "tp", axis=0, tiled=True)
    wide = lax.all_to_all(tall, "fs", 0, 1, tiled=True)
    columns = wide.shape[1] // tp
    return lax.dynamic_slice_in_dim(wide, lax.axis_index("tp") * columns, columns, 1)


def normed_rows(block, gain, fs):
    values = block.astype(jnp.float32)
    width = block.shape[1]
    square = lax.psum(jnp.sum(values * values, axis=1), "fs") / (width * fs)
    own = lax.dynamic_slice_in_dim(gain, lax.axis_index("fs") * width, width, 0)
    scaled = (values * lax.rsqrt(square + epsilon)[:, None] * own).astype(jnp.bfloat16)
    return lax.all_gather(scaled, "tp", axis=0, tiled=True)


def solution(mesh):
    fs, tp = mesh.shape["fs"], mesh.shape["tp"]

    def on_device(
        tokens,
        mixer_gain,
        gate_proj,
        value_proj,
        value_gain,
        spatial_mix,
        spatial_bias,
        head_gain,
        merge_proj,
        ffn_gain,
        gate_up,
        value_up,
        gate_kernel,
        value_kernel,
        gate_offset,
        value_offset,
        down_proj,
    ):
        heads_here = spatial_mix.shape[0]
        length = spatial_mix.shape[2]
        width = gate_proj.shape[1]
        head_width = width // heads_here
        rows = tokens.shape[0]
        seqs = rows // length
        matrix = lax.all_gather(spatial_mix, "fs", axis=1, tiled=True)

        turned = swap(tokens, fs, tp)
        normed = normed_rows(turned, mixer_gain, fs)
        both = jnp.concatenate([dot(normed, gate_proj), dot(normed, value_proj)], axis=1)
        both = lax.psum_scatter(both, "fs", scatter_dimension=0, tiled=True).astype(jnp.float32)
        gated = gelu_exact(both[:, :width])
        spread = gelu_exact(both[:, width:])
        spread = normalize(spread.reshape(seqs, length, heads_here, head_width), value_gain).astype(
            jnp.bfloat16
        )
        mixed = jnp.einsum("hij,njhd->nihd", matrix, spread, preferred_element_type=jnp.float32)
        mixed = mixed + spatial_bias.T[None, :, :, None]
        joined = gated.reshape(seqs, length, heads_here, head_width) * mixed
        merged = normalize(joined, head_gain).astype(jnp.bfloat16).reshape(rows, width)

        merged = lax.all_gather(merged, "fs", axis=0, tiled=True)
        branch = lax.psum_scatter(dot(merged, merge_proj), "tp", scatter_dimension=0, tiled=True)
        hidden = (turned.astype(jnp.float32) + branch.astype(jnp.float32)).astype(jnp.bfloat16)

        normed_ffn = normed_rows(hidden, ffn_gain, fs)
        upper_gate = lax.psum_scatter(dot(normed_ffn, gate_up), "fs", scatter_dimension=0, tiled=True)
        upper_value = lax.psum_scatter(dot(normed_ffn, value_up), "fs", scatter_dimension=0, tiled=True)
        conv_gate = convolve(upper_gate.astype(jnp.float32), gate_kernel, gate_offset, length)
        conv_value = convolve(upper_value.astype(jnp.float32), value_kernel, value_offset, length)
        active = (gelu_exact(conv_gate) * conv_value).astype(jnp.bfloat16)

        active = lax.all_gather(active, "fs", axis=0, tiled=True)
        change = lax.psum_scatter(dot(active, down_proj), "tp", scatter_dimension=0, tiled=True)
        result = (hidden.astype(jnp.float32) + change.astype(jnp.float32)).astype(jnp.bfloat16)
        return swap_back(result, fs, tp)

    in_specs = (
        P(("rep", "fs"), "tp"),
        P(),
        P("fs", "tp"),
        P("fs", "tp"),
        P("tp", None),
        P("tp", "fs", None),
        P("tp", None),
        P("tp", None),
        P("tp", "fs"),
        P(),
        P("fs", "tp"),
        P("fs", "tp"),
        P(None, "tp"),
        P(None, "tp"),
        P("tp"),
        P("tp"),
        P("tp", "fs"),
    )
    out_specs = P(("rep", "fs"), "tp")
    return jax.shard_map(
        on_device, mesh=mesh, in_specs=in_specs, out_specs=out_specs, check_vma=False
    )
```
